32 devices in a mesh: sp: 8 (over z, y), tp: 4 (over x, core).
Axes of the slice: x: 2, y: 2, z: 4, core: 2. Of those that a mesh axis runs over, the one named last changes fastest.
Arguments:
- latent: bfloat16 [2048, 2048], P(('sp', 'tp')), may hold values from -6 to 6
- log_decay: float32 [2048, 8], P('sp', 'tp'), may hold values from -2 to 0
- context: bfloat16 [128, 2048], P('sp'), may hold values from -6 to 6
- condition: bfloat16 [2, 2048], replicated, may hold values from -6 to 6
- w_modulate: bfloat16 [2048, 6144], P('sp', 'tp'), may hold values from -1 to 1
- norm_gain: bfloat16 [2048], replicated, may hold values from 0.099609375 to 1.8984375
- w_query: bfloat16 [2048, 2048], P(None, 'tp'), may hold values from -0.125 to 0.125
- w_key: bfloat16 [2048, 2048], P(None, 'tp'), may hold values from -0.125 to 0.125
- w_value: bfloat16 [2048, 4096], P(None, 'tp'), may hold values from -0.125 to 0.125
- w_gate: bfloat16 [2048, 4096], P(None, 'tp'), may hold values from -0.125 to 0.125
- group_gain: bfloat16 [4096], P('tp'), may hold values from 0.099609375 to 1.8984375
- w_output: bfloat16 [4096, 2048], P('tp'), may hold values from -0.125 to 0.125
Outputs:
- updated: bfloat16 [2048, 2048], P(('sp', 'tp'))
The draws below stay inside these ranges and needn't reach their ends.
All inputs are finite; a program needn't handle non-finite values.
Results may differ from the reference program's by a relative error of at most 0.014.
Values may be sent and summed in bfloat16 or wider, within the bound.
A program may use at most 128 MiB of HBM per device.

```python
import math
import jax
import jax.numpy as jnp
from jax import lax

D = 2048
RETENTION_HEADS = 8
DK = 256
DV = 512
BLOCK = 128
GRID_W = 64
LATENT_TOKENS = 2048
CTX = 128
CTX_LIFT = 4
N_TP = 4


def draw_log_decay(key, part):
    random_keys = jax.random.split(key, 7)
    fast_count = max(1, RETENTION_HEADS // 4)
    head_order = jax.random.permutation(random_keys[0], RETENTION_HEADS)
    quick_decay_heads = head_order < fast_count
    slow_rate = jax.random.uniform(random_keys[1], (RETENTION_HEADS,), jnp.float32, 0.1, 0.4) * math.log(10.0) / LATENT_TOKENS
    fast_rate = jax.random.uniform(random_keys[2], (RETENTION_HEADS,), jnp.float32, 4.0, 8.0) / BLOCK
    base_rate = jnp.where(quick_decay_heads, fast_rate, slow_rate)
    block_count = LATENT_TOKENS // BLOCK
    block_factor = jnp.exp(jax.random.uniform(random_keys[3], (block_count, 1, RETENTION_HEADS), jnp.float32, math.log(0.4), math.log(1.6)))
    jitter = jax.random.uniform(random_keys[4], (block_count, BLOCK, RETENTION_HEADS), jnp.float32, 0.5, 1.5)
    decay_rates = (base_rate * block_factor * jitter).reshape(LATENT_TOKENS, RETENTION_HEADS)
    spike_positions = jax.random.randint(random_keys[5], (2,), 0, LATENT_TOKENS)
    spike_lengths = jax.random.uniform(random_keys[6], (2, RETENTION_HEADS), jnp.float32, 0.22, 0.51)
    spike_flags = (jnp.arange(LATENT_TOKENS)[:, None] == spike_positions[None, :]).astype(jnp.float32)
    spike_runs = jnp.dot(spike_flags, spike_lengths) * jnp.where(quick_decay_heads, 0.0, 1.0)
    return (-(decay_rates + spike_runs)).astype(jnp.float32)


def draw_latent(key, part):
    random_keys = jax.random.split(key, 1)
    drawn = jnp.clip(jax.random.normal(random_keys[0], (LATENT_TOKENS, D), jnp.float32), -6.0, 6.0)
    return drawn.astype(jnp.bfloat16)


def draw_w_modulate(key, part):
    column_scale = jnp.concatenate([jnp.full((D,), 0.12, jnp.float32), jnp.ones((2 * D,), jnp.float32)]) * math.sqrt(2.0 / D)
    base_values = jax.random.normal(key, (D, 3 * D), jnp.float32)
    return jnp.clip(base_values * column_scale[None, :], -1.0, 1.0).astype(jnp.bfloat16)


def level_of(rng, shape, pieces, least, top_value):
    factor_of = 1.0
    for axis_at, blocks in pieces:
        draws = jax.random.uniform(jax.random.fold_in(jax.random.fold_in(rng, 6), axis_at), (blocks,), jnp.float32, least / len(pieces), top_value / len(pieces))
        factor_of = factor_of * jnp.repeat(jnp.exp(draws), shape[axis_at] // blocks).reshape((-1,) + (1,) * (len(shape) - 1 - axis_at))
    return factor_of


def bell_draw(stream_key, shape, spread, reach, cuts=(), kind=jnp.bfloat16):
    result = spread * jax.random.normal(stream_key, shape, jnp.float32)
    if cuts:
        result = result * level_of(stream_key, shape, cuts, -0.22, 0.18)
    return jnp.clip(result, -reach, reach).astype(kind)


def setup_inputs(seed: int = 0) -> dict:
    splits = jax.random.split(jax.random.key(seed), 13)
    latent = draw_latent(jax.random.fold_in(splits[12], 71), 0)
    log_decay = draw_log_decay(jax.random.fold_in(splits[12], 71), 0)
    context = bell_draw(splits[2], (CTX, D), 1.0, 6.0, ((0, 8),))
    condition = bell_draw(splits[3], (2, D), 1.0, 6.0)
    w_modulate = draw_w_modulate(jax.random.fold_in(splits[12], 71), 0)
    norm_gain = jnp.clip(1.0 + 0.18 * jax.random.normal(splits[5], (D,), jnp.float32), 0.099609375, 1.8984375).astype(jnp.bfloat16)
    w_query = bell_draw(splits[6], (D, D), D ** -0.5, 0.125, ((1, 4),))
    w_key = bell_draw(splits[7], (D, D), D ** -0.5, 0.125, ((1, 4),))
    w_value = bell_draw(splits[8], (D, 2 * D), D ** -0.5, 0.125, ((1, 4),))
    w_gate = bell_draw(splits[9], (D, 2 * D), D ** -0.5, 0.125, ((1, 4),))
    group_gain = jnp.clip(1.0 + 0.18 * jax.random.normal(splits[10], (2 * D,), jnp.float32), 0.099609375, 1.8984375).astype(jnp.bfloat16)
    w_output = bell_draw(splits[11], (2 * D, D), D ** -0.5, 0.125, ((0, 4),))
    return dict(latent=latent, log_decay=log_decay, context=context, condition=condition, w_modulate=w_modulate, norm_gain=norm_gain, w_query=w_query, w_key=w_key, w_value=w_value, w_gate=w_gate, group_gain=group_gain, w_output=w_output)


epsilon = 1e-06
rotary_base = 10000.0

def modulate_rows(row_block, norm_gain, shift_vec, scale_vec):
    wide = row_block.astype(jnp.float32)
    normal = wide * lax.rsqrt(lax.optimization_barrier(jnp.mean(wide * wide, axis=-1, keepdims=True)) + epsilon)
    return (normal * norm_gain.astype(jnp.float32) * (1.0 + scale_vec) + shift_vec).astype(jnp.bfloat16)

def rotate(projected, positions):
    pairs = DK // 4
    inverse = rotary_base ** (-jnp.arange(pairs, dtype=jnp.float32) / pairs)
    grid_row = (positions // GRID_W).astype(jnp.float32)
    grid_column = (positions % GRID_W).astype(jnp.float32)
    angles = jnp.concatenate([grid_row[:, None] * inverse, grid_column[:, None] * inverse], axis=-1)
    cosine = jnp.cos(angles)[:, None, :]
    sine_part = jnp.sin(angles)[:, None, :]
    paired = projected.reshape(projected.shape[0], -1, DK // 2, 2)
    even_part = paired[..., 0]
    odd_part = paired[..., 1]
    turned = jnp.stack([even_part * cosine - odd_part * sine_part, even_part * sine_part + odd_part * cosine], axis=-1)
    return turned.reshape(projected.shape)

def narrowed(values):
    return lax.optimization_barrier(values.astype(jnp.bfloat16)).astype(jnp.float32)

def sweep_blocks(queries, key_rows, value_rows, decays, entry):
    block_count = queries.shape[0] // BLOCK
    head_count = queries.shape[1]

    def advance(states, element):
        query_block, key_block, value_block, decay_block = element
        cumulative = jnp.cumsum(decay_block, axis=0)
        by_head = cumulative.T
        within = jnp.arange(BLOCK, dtype=jnp.int32)
        lower_mask = within[:, None] >= within[None, :]
        log_gaps = by_head[:, :, None] - by_head[:, None, :]
        weights = jnp.where(lower_mask, jnp.exp(jnp.where(lower_mask, log_gaps, 0.0)), 0.0)
        query_wide = query_block.astype(jnp.float32)
        value_wide = value_block.astype(jnp.float32)
        scores = jnp.einsum('ihd,jhd->hij', query_wide, key_block.astype(jnp.float32))
        weighted = narrowed(scores * weights)
        inside = jnp.einsum('hij,jhv->ihv', weighted, value_wide)
        carried_in = jnp.exp(cumulative)[:, :, None] * jnp.einsum('ihd,hdv->ihv', query_wide, narrowed(states))
        totals = cumulative[-1]
        decayed = narrowed(key_block.astype(jnp.float32) * jnp.exp(totals[None, :] - cumulative)[:, :, None])
        updates = jnp.einsum('jhd,jhv->hdv', decayed, value_wide)
        return (jnp.exp(totals)[:, None, None] * states + updates, inside + carried_in)
    blocks = (queries.reshape(block_count, BLOCK, head_count, DK), key_rows.reshape(block_count, BLOCK, head_count, DK), value_rows.reshape(block_count, BLOCK, head_count, DV), decays.reshape(block_count, BLOCK, head_count))
    unused, outputs = lax.scan(advance, entry, blocks)
    return outputs.reshape(queries.shape[0], head_count, DV)

def reference(latent, log_decay, context, condition, w_modulate, norm_gain, w_query, w_key, w_value, w_gate, group_gain, w_output):
    activated = jax.nn.silu(condition.astype(jnp.float32)).astype(jnp.bfloat16)
    modulation = jnp.dot(activated, w_modulate, preferred_element_type=jnp.float32)
    normed = modulate_rows(latent, norm_gain, modulation[0, :D], modulation[0, D:2 * D])
    context_normed = modulate_rows(context, norm_gain, modulation[1, :D], modulation[1, D:2 * D])
    positions = jnp.arange(LATENT_TOKENS, dtype=jnp.int32)
    query_rows = rotate(jnp.dot(normed, w_query, preferred_element_type=jnp.float32), positions).astype(jnp.bfloat16)
    key_rows = (rotate(jnp.dot(normed, w_key, preferred_element_type=jnp.float32), positions) * DK ** (-0.5)).astype(jnp.bfloat16)
    value_rows = jnp.dot(normed, w_value, preferred_element_type=jnp.float32).astype(jnp.bfloat16)
    gate_rows = jnp.dot(normed, w_gate, preferred_element_type=jnp.float32).astype(jnp.bfloat16)
    context_keys = (jnp.dot(context_normed, w_key, preferred_element_type=jnp.float32) * DK ** (-0.5)).astype(jnp.bfloat16)
    context_values = jnp.dot(context_normed, w_value, preferred_element_type=jnp.float32).astype(jnp.bfloat16)
    context_state = jnp.einsum('jhd,jhv->hdv', context_keys.reshape(CTX, RETENTION_HEADS, DK).astype(jnp.float32), context_values.reshape(CTX, RETENTION_HEADS, DV).astype(jnp.float32)) * float(CTX_LIFT)
    queries = query_rows.reshape(LATENT_TOKENS, RETENTION_HEADS, DK)
    key_heads = key_rows.reshape(LATENT_TOKENS, RETENTION_HEADS, DK)
    value_heads = value_rows.reshape(LATENT_TOKENS, RETENTION_HEADS, DV)
    forward = sweep_blocks(queries, key_heads, value_heads, log_decay, context_state)
    backward = jnp.flip(sweep_blocks(jnp.flip(queries, 0), jnp.flip(key_heads, 0), jnp.flip(value_heads, 0), jnp.flip(log_decay, 0), context_state), 0)
    mixed_heads = forward + backward
    average = lax.optimization_barrier(jnp.mean(mixed_heads, axis=-1, keepdims=True))
    variance = lax.optimization_barrier(jnp.mean(jnp.square(mixed_heads - average), axis=-1, keepdims=True))
    normal_heads = ((mixed_heads - average) * lax.rsqrt(variance + epsilon)).reshape(LATENT_TOKENS, RETENTION_HEADS * DV)
    attended = (jax.nn.silu(gate_rows.astype(jnp.float32)) * normal_heads * group_gain.astype(jnp.float32)).astype(jnp.bfloat16)
    group_width = attended.shape[1] // N_TP
    projected = jnp.zeros((LATENT_TOKENS, D), jnp.float32)
    for group in range(N_TP):
        partial_sum = jnp.dot(attended[:, group * group_width:(group + 1) * group_width], w_output[group * group_width:(group + 1) * group_width], preferred_element_type=jnp.float32)
        projected = projected + narrowed(partial_sum)
    return (latent.astype(jnp.float32) + modulation[0, 2 * D:] * projected).astype(jnp.bfloat16)
```

```python
import functools

import jax
import jax.numpy as jnp
import numpy as np
from jax import lax
from jax.experimental import pallas as pl
from jax.experimental.pallas import tpu as pltpu
from jax.sharding import PartitionSpec as P

DK = 256
DV = 512
GRID_W = 64
CTX_LIFT = 4
CORES = 2
CHUNKS = 4

epsilon = 1e-06
rotary_base = 10000.0
MESH = pl.DeviceIdType.MESH
F32 = jnp.float32
BF16 = jnp.bfloat16


def silu(v):
    return v / (1.0 + jnp.exp(-v))


def rotary_tables(grid_rows):
    pairs = DK // 4
    inverse = (rotary_base ** (-np.arange(pairs, dtype=np.float64) / pairs)).astype(np.float32)

    def tables(count):
        angles = (np.arange(count, dtype=np.float32)[:, None] * inverse[None, :]).astype(np.float32)
        cosine = np.repeat(np.cos(angles.astype(np.float64)), 2, axis=1)
        sine = np.repeat(np.sin(angles.astype(np.float64)), 2, axis=1)
        sine[:, 0::2] *= -1.0
        return cosine.astype(np.float32), sine.astype(np.float32)

    return tables(grid_rows) + tables(GRID_W)


def kernel(
    n_sp, n_tp, group, rows, head_count,
    lat_ref, dec_ref, ctx_ref, cond_ref, ngain_ref, ggain_ref,
    rowc_ref, rows_ref, colc_ref, cols_ref,
    wmod_hbm, wq_hbm, wk_hbm, wv_hbm, wg_hbm, wo_hbm,
    out_ref,
    wmod, wk, wv, wq, wg, wo,
    lat_all, normed, ctx_all, dec_all, mslots, modfull,
    wdec, vecs, etot,
    kbuf, qbuf, vbuf, gbuf, ybuf, fstate, bstate,
    recv_f, recv_b, send_f, send_b,
    att, pout, pin, psend, pfin,
    w_sem, dec_s, dec_r, m1_s, m1_r, m2_s, m2_r, lat_s, lat_r, rel_s, rel_r,
    ctx_s, ctx_r, f_s, f_r, b_s, b_r, d2d_s, d2d_r, ici_s, ici_r,
):
    sp = lax.axis_index("sp")
    tp = lax.axis_index("tp")
    zz = sp // group
    sub = sp % group
    nz = n_sp // group
    members = group * n_tp
    chips = members // CORES
    me = sub * n_tp + tp
    chip = me // CORES
    core = me % CORES
    tokens = members * rows
    model = lat_ref.shape[1]

    def member_device(m):
        return (zz * group + m // n_tp, m % n_tp)

    partner = member_device(chip * CORES + (1 - core))

    def remote(src, dst, ssem, rsem, device):
        return pltpu.make_async_remote_copy(
            src_ref=src, dst_ref=dst, send_sem=ssem, recv_sem=rsem,
            device_id=device, device_id_type=MESH,
        )

    key_cols = pl.ds(pl.multiple_of(sub * DK, DK), DK)
    val_cols = pl.ds(pl.multiple_of(sub * DV, DV), DV)
    loads = [
        pltpu.make_async_copy(wmod_hbm, wmod, w_sem.at[0]),
        pltpu.make_async_copy(wk_hbm.at[:, key_cols], wk, w_sem.at[1]),
        pltpu.make_async_copy(wv_hbm.at[:, val_cols], wv, w_sem.at[2]),
        pltpu.make_async_copy(wq_hbm.at[:, key_cols], wq, w_sem.at[3]),
        pltpu.make_async_copy(wg_hbm.at[:, val_cols], wg, w_sem.at[4]),
        pltpu.make_async_copy(wo_hbm.at[val_cols, :], wo, w_sem.at[5]),
    ]
    for load in loads:
        load.start()

    barrier = pltpu.get_barrier_semaphore()
    greeted = 0
    for d in range(1, n_sp):
        pl.semaphore_signal(
            barrier, inc=1, device_id=((sp + d) % n_sp, tp), device_id_type=MESH
        )
        greeted += 1
    for s in range(group):
        for d in range(1, n_tp):
            pl.semaphore_signal(
                barrier, inc=1, device_id=(zz * group + s, (tp + d) % n_tp), device_id_type=MESH
            )
            greeted += 1
    pl.semaphore_wait(barrier, greeted)

    sends = []

    depth, width = wmod.shape
    if cond_ref.shape[1] == depth:
        own = cond_ref[...]
    else:
        own = cond_ref[:, pl.ds(pl.multiple_of(sp * depth, depth), depth)]
    activated = silu(own.astype(F32)).astype(BF16)
    loads[0].wait()
    mslots[sp] = jnp.dot(activated, wmod[...], preferred_element_type=F32)
    first = []
    for d in range(1, n_sp):
        copy = remote(
            mslots.at[sp], mslots.at[sp], m1_s.at[d], m1_r.at[d], ((sp + d) % n_sp, tp)
        )
        copy.start()
        first.append(copy)
    sends += first

    decay_copies = []
    for d in range(1, group):
        copy = remote(
            dec_ref, dec_all.at[sub], dec_s.at[d], dec_r.at[d],
            (zz * group + (sub + d) % group, tp),
        )
        copy.start()
        decay_copies.append(copy)
    sends += decay_copies
    dec_all[sub] = dec_ref[...]

    lat_copies = []
    for d in range(1, chips):
        copy = remote(
            lat_ref, lat_all.at[me], lat_s.at[d], lat_r.at[d],
            member_device(((chip + d) % chips) * CORES + core),
        )
        copy.start()
        lat_copies.append(copy)
    sends += lat_copies
    own_relay = remote(lat_ref, lat_all.at[me], rel_s.at[0], rel_r.at[0], partner)
    own_relay.start()
    relays = [own_relay]
    lat_all[me] = lat_ref[...]

    ends = sorted({0, nz - 1})
    ctx_sends = []
    for e in ends:
        for s in range(group):
            dest = e * group + s
            slot = len(ctx_sends)

            def ctx_copy(dest=dest, slot=slot):
                return remote(ctx_ref, ctx_all.at[sp], ctx_s.at[slot], ctx_r.at[sp], (dest, tp))

            @pl.when(sp != dest)
            def _(ctx_copy=ctx_copy):
                ctx_copy().start()

            ctx_sends.append((dest, ctx_copy))
    ctx_all[sp] = ctx_ref[...]

    for copy in first:
        copy.wait_recv()
    total = mslots[0]
    for s in range(1, n_sp):
        total = total + mslots[s]
    mod_cols = pl.ds(pl.multiple_of(tp * width, width), width)
    modfull[:, mod_cols] = total
    second = []
    for d in range(1, n_tp):
        copy = remote(
            modfull.at[:, mod_cols], modfull.at[:, mod_cols], m2_s.at[d], m2_r.at[d],
            (sp, (tp + d) % n_tp),
        )
        copy.start()
        second.append(copy)
    sends += second

    for copy in decay_copies:
        copy.wait_recv()
    head = sub if head_count > 1 else 0
    parts = [dec_all[s, pl.ds(head, 1), :] for s in range(group)]
    a_row = parts[0] if group == 1 else jnp.concatenate(parts, axis=1)
    ii = lax.broadcasted_iota(jnp.int32, (tokens, tokens), 0)
    jj = lax.broadcasted_iota(jnp.int32, (tokens, tokens), 1)
    a_full = jnp.broadcast_to(a_row, (tokens, tokens))
    b_col = jnp.sum(jnp.where(jj <= ii, a_full, 0.0), axis=1, keepdims=True)
    a_col = jnp.sum(jnp.where(jj == ii, a_full, 0.0), axis=1, keepdims=True)
    c_col = b_col - a_col
    b_row = jnp.sum(jnp.where(jj == ii, b_col, 0.0), axis=0, keepdims=True)
    c_row = jnp.sum(jnp.where(jj == ii, c_col, 0.0), axis=0, keepdims=True)
    gap = jnp.where(jj <= ii, b_col - b_row, c_row - c_col)
    wdec[...] = jnp.where(jj == ii, 2.0, jnp.exp(jnp.minimum(gap, 0.0)))
    t_all = b_col[tokens - 1 : tokens, :]
    vecs[0] = jnp.exp(b_col)
    vecs[1] = jnp.exp(t_all - c_col)
    vecs[2] = jnp.exp(t_all - b_col)
    vecs[3] = jnp.exp(c_col)
    etot[...] = jnp.broadcast_to(jnp.exp(t_all), etot.shape)

    for d in range(1, chips):
        lat_copies[d - 1].wait_recv()
        source = ((chip + chips - d) % chips) * CORES + core
        copy = remote(lat_all.at[source], lat_all.at[source], rel_s.at[d], rel_r.at[d], partner)
        copy.start()
        relays.append(copy)
    sends += relays

    for copy in second:
        copy.wait_recv()
    for copy in relays:
        copy.wait_recv()

    gain = ngain_ref[...]

    def modulate(x, row):
        wide = x.astype(F32)
        normal = wide * lax.rsqrt(jnp.mean(wide * wide, axis=-1, keepdims=True) + epsilon)
        shift = modfull[row : row + 1, 0:model]
        scale = modfull[row : row + 1, model : 2 * model]
        return (normal * gain * (1.0 + scale) + shift).astype(BF16)

    @pl.loop(0, members)
    def _(m):
        normed[m] = modulate(lat_all[m], 0)

    x = normed[...].reshape(tokens, model)
    lanes = lax.broadcasted_iota(jnp.int32, (GRID_W, DK // 2), 1)
    even = lanes % 2 == 0
    row_base = zz * (tokens // GRID_W)

    def rotate_into(dst, scale):
        for r in range(tokens // GRID_W):
            at = slice(r * GRID_W, (r + 1) * GRID_W)
            row_c = rowc_ref[pl.ds(row_base + r, 1), :]
            row_s = rows_ref[pl.ds(row_base + r, 1), :]
            for part in range(2):
                cut = slice(part * (DK // 2), (part + 1) * (DK // 2))
                u = ybuf[at, cut]
                swapped = jnp.where(
                    even, pltpu.roll(u, DK // 2 - 1, 1), pltpu.roll(u, 1, 1)
                )
                if part == 0:
                    turned = u * row_c + swapped * row_s
                else:
                    turned = u * colc_ref[...] + swapped * cols_ref[...]
                dst[at, cut] = (turned * scale).astype(BF16)

    loads[1].wait()
    ybuf[:, 0:DK] = jnp.dot(x, wk[...], preferred_element_type=F32)
    rotate_into(kbuf, DK ** (-0.5))
    loads[2].wait()
    for n in range(DV // 256):
        cut = slice(n * 256, (n + 1) * 256)
        vbuf[:, cut] = jnp.dot(x, wv[:, cut], preferred_element_type=F32).astype(BF16)

    over_tokens = (((0,), (0,)), ((), ()))

    @pl.when((zz == 0) | (zz == nz - 1))
    def _():
        for s in range(n_sp):
            @pl.when(sp != s)
            def _(s=s):
                remote(
                    ctx_ref, ctx_all.at[s], ctx_s.at[0], ctx_r.at[s], (sp, tp)
                ).wait_recv()
        cn = modulate(ctx_all[...].reshape(-1, model), 1)
        ck = (jnp.dot(cn, wk[...], preferred_element_type=F32) * DK ** (-0.5)).astype(BF16)
        cv = jnp.dot(cn, wv[...], preferred_element_type=F32).astype(BF16)
        state = lax.dot_general(ck, cv, over_tokens, preferred_element_type=F32) * float(CTX_LIFT)
        state = state.astype(BF16).reshape(recv_f.shape)

        @pl.when(zz == 0)
        def _():
            recv_f[...] = state

        @pl.when(zz == nz - 1)
        def _():
            recv_b[...] = state

    v = vbuf[...]
    kw = kbuf[...].astype(F32)
    fstate[...] = lax.dot_general(
        (kw * vecs[2]).astype(BF16), v, over_tokens, preferred_element_type=F32
    )
    bstate[...] = lax.dot_general(
        (kw * vecs[3]).astype(BF16), v, over_tokens, preferred_element_type=F32
    )

    piece = DK // CHUNKS

    def f_copy(c):
        return remote(
            send_f.at[c], recv_f.at[c], f_s.at[c], f_r.at[c], ((sp + group) % n_sp, tp)
        )

    def b_copy(c):
        return remote(
            send_b.at[c], recv_b.at[c], b_s.at[c], b_r.at[c], ((sp + n_sp - group) % n_sp, tp)
        )

    def chain_f():
        for c in range(CHUNKS):
            @pl.when(zz > 0)
            def _(c=c):
                f_copy(c).wait_recv()

            @pl.when(zz < nz - 1)
            def _(c=c):
                cut = slice(c * piece, (c + 1) * piece)
                send_f[c] = (etot[...] * recv_f[c].astype(F32) + fstate[cut, :]).astype(BF16)
                f_copy(c).start()

    def chain_b():
        for c in range(CHUNKS):
            @pl.when(zz < nz - 1)
            def _(c=c):
                b_copy(c).wait_recv()

            @pl.when(zz > 0)
            def _(c=c):
                cut = slice(c * piece, (c + 1) * piece)
                send_b[c] = (etot[...] * recv_b[c].astype(F32) + bstate[cut, :]).astype(BF16)
                b_copy(c).start()

    @pl.when(2 * zz < nz)
    def _():
        chain_f()

    @pl.when(2 * zz >= nz)
    def _():
        chain_b()

    loads[3].wait()
    ybuf[:, 0:DK] = jnp.dot(x, wq[...], preferred_element_type=F32)
    rotate_into(qbuf, 1.0)
    q = qbuf[...]
    scores = lax.dot_general(
        q, kbuf[...], (((1,), (1,)), ((), ())), preferred_element_type=F32
    )
    ybuf[...] = jnp.dot((scores * wdec[...]).astype(BF16), v, preferred_element_type=F32)

    @pl.when(2 * zz < nz)
    def _():
        chain_b()

    @pl.when(2 * zz >= nz)
    def _():
        chain_f()

    loads[4].wait()
    for n in range(DV // 256):
        cut = slice(n * 256, (n + 1) * 256)
        g = jnp.dot(x, wg[:, cut], preferred_element_type=F32).astype(BF16)
        gbuf[:, cut] = silu(g.astype(F32)) * ggain_ref[
            :, pl.ds(pl.multiple_of(sub * DV + n * 256, 256), 256)
        ]

    y = ybuf[...]
    y = y + vecs[0] * jnp.dot(q, recv_f[...].reshape(DK, DV), preferred_element_type=F32)
    y = y + vecs[1] * jnp.dot(q, recv_b[...].reshape(DK, DV), preferred_element_type=F32)
    ybuf[...] = y

    @pl.loop(0, chips)
    def _(c):
        span = CORES * rows
        at = pl.ds(pl.multiple_of(c * span, span), span)
        part = ybuf[at, :]
        centred = part - jnp.mean(part, axis=-1, keepdims=True)
        variance = jnp.mean(centred * centred, axis=-1, keepdims=True)
        att[c] = (gbuf[at, :] * (centred * lax.rsqrt(variance + epsilon))).astype(BF16)

    loads[5].wait()
    order = list(range(1, chips)) + [0]
    pair_copies = {}
    final = {}

    def finish(d):
        pair_copies[d].wait_recv()
        both = pout[d, core].astype(F32) + pin[d].astype(F32)
        if d == 0:
            final["own"] = both
            return
        psend[d] = both.astype(BF16)
        copy = remote(
            psend.at[d], pfin.at[d], ici_s.at[d], ici_r.at[d],
            member_device(((chip + d) % chips) * CORES + core),
        )
        copy.start()
        final[d] = copy
        sends.append(copy)

    for place, d in enumerate(order):
        rows_of = att[(chip + d) % chips]
        pout[d] = (
            jnp.dot(rows_of, wo[...], preferred_element_type=F32)
            .astype(BF16)
            .reshape(CORES, rows, model)
        )
        copy = remote(pout.at[d, 1 - core], pin.at[d], d2d_s.at[d], d2d_r.at[d], partner)
        copy.start()
        pair_copies[d] = copy
        sends.append(copy)
        if place:
            finish(order[place - 1])
    finish(order[-1])
    acc = final["own"]
    for d in range(1, chips):
        final[d].wait_recv()
        acc = acc + pfin[d].astype(F32)
    gate = modfull[0:1, 2 * model : 3 * model]
    out_ref[...] = (lat_ref[...].astype(F32) + gate * acc).astype(BF16)

    for copy in sends:
        copy.wait_send()
    for dest, ctx_copy in ctx_sends:
        @pl.when(sp != dest)
        def _(ctx_copy=ctx_copy):
            ctx_copy().wait_send()

    @pl.when(zz < nz - 1)
    def _():
        for c in range(CHUNKS):
            f_copy(c).wait_send()

    @pl.when(zz > 0)
    def _():
        for c in range(CHUNKS):
            b_copy(c).wait_send()


def per_device(
    n_sp, n_tp,
    latent, log_decay, context, condition, w_modulate, norm_gain,
    w_query, w_key, w_value, w_gate, group_gain, w_output,
):
    rows, model = latent.shape
    head_count = w_query.shape[1] // DK
    group = head_count
    members = group * n_tp
    chips = members // CORES
    tokens = members * rows
    depth, width = w_modulate.shape
    ctx_rows = context.shape[0]
    if depth % 128:
        condition = lax.dynamic_slice_in_dim(condition, lax.axis_index("sp") * depth, depth, 1)
    total_rows = rows * n_sp * n_tp
    tables = [jnp.asarray(t) for t in rotary_tables(total_rows // GRID_W)]
    vmem = pl.BlockSpec(memory_space=pltpu.VMEM)
    hbm = pl.BlockSpec(memory_space=pl.ANY)
    sem = pltpu.SemaphoreType.DMA
    ends = 2 * group
    scratch = [
        pltpu.VMEM((depth, width), BF16),
        pltpu.VMEM((model, DK), BF16),
        pltpu.VMEM((model, DV), BF16),
        pltpu.VMEM((model, DK), BF16),
        pltpu.VMEM((model, DV), BF16),
        pltpu.VMEM((DV, model), BF16),
        pltpu.VMEM((members, rows, model), BF16),
        pltpu.VMEM((members, rows, model), BF16),
        pltpu.VMEM((n_sp, ctx_rows, model), BF16),
        pltpu.VMEM((group, head_count, log_decay.shape[0]), F32),
        pltpu.VMEM((n_sp, condition.shape[0], width), F32),
        pltpu.VMEM((condition.shape[0], width * n_tp), F32),
        pltpu.VMEM((tokens, tokens), F32),
        pltpu.VMEM((4, tokens, 1), F32),
        pltpu.VMEM((1, DV), F32),
        pltpu.VMEM((tokens, DK), BF16),
        pltpu.VMEM((tokens, DK), BF16),
        pltpu.VMEM((tokens, DV), BF16),
        pltpu.VMEM((tokens, DV), F32),
        pltpu.VMEM((tokens, DV), F32),
        pltpu.VMEM((DK, DV), F32),
        pltpu.VMEM((DK, DV), F32),
        pltpu.VMEM((CHUNKS, DK // CHUNKS, DV), BF16),
        pltpu.VMEM((CHUNKS, DK // CHUNKS, DV), BF16),
        pltpu.VMEM((CHUNKS, DK // CHUNKS, DV), BF16),
        pltpu.VMEM((CHUNKS, DK // CHUNKS, DV), BF16),
        pltpu.VMEM((chips, CORES * rows, DV), BF16),
        pltpu.VMEM((chips, CORES, rows, model), BF16),
        pltpu.VMEM((chips, rows, model), BF16),
        pltpu.VMEM((chips, rows, model), BF16),
        pltpu.VMEM((chips, rows, model), BF16),
        sem((6,)),
        sem((group,)), sem((group,)),
        sem((n_sp,)), sem((n_sp,)),
        sem((n_tp,)), sem((n_tp,)),
        sem((chips,)), sem((chips,)),
        sem((chips,)), sem((chips,)),
        sem((ends,)), sem((n_sp,)),
        sem((CHUNKS,)), sem((CHUNKS,)),
        sem((CHUNKS,)), sem((CHUNKS,)),
        sem((chips,)), sem((chips,)),
        sem((chips,)), sem((chips,)),
    ]
    return pl.pallas_call(
        functools.partial(kernel, n_sp, n_tp, group, rows, head_count),
        out_shape=jax.ShapeDtypeStruct((rows, model), BF16),
        in_specs=[vmem] * 10 + [hbm] * 6,
        out_specs=vmem,
        scratch_shapes=scratch,
        compiler_params=pltpu.CompilerParams(
            collective_id=0, has_side_effects=True, vmem_limit_bytes=58 * 1024 * 1024
        ),
    )(
        latent, log_decay.T, context, condition,
        norm_gain.astype(F32).reshape(1, -1), group_gain.astype(F32).reshape(1, -1),
        *tables,
        w_modulate, w_query, w_key, w_value, w_gate, w_output,
    )


def solution(mesh):
    placed = (
        P(("sp", "tp"), None),
        P("sp", "tp"),
        P("sp", None),
        P(),
        P("sp", "tp"),
        P(),
        P(None, "tp"),
        P(None, "tp"),
        P(None, "tp"),
        P(None, "tp"),
        P("tp"),
        P("tp", None),
    )
    body = functools.partial(per_device, mesh.shape["sp"], mesh.shape["tp"])
    return jax.shard_map(
        body, mesh=mesh, in_specs=placed, out_specs=P(("sp", "tp"), None), check_vma=False
    )
```

```python
import functools

import jax
import jax.numpy as jnp
import numpy as np
from jax import lax
from jax.experimental import pallas as pl
from jax.experimental.pallas import tpu as pltpu
from jax.sharding import PartitionSpec as P

DK = 256
DV = 512
GRID_W = 64
CTX_LIFT = 4
CORES = 2
CHUNKS = 4

epsilon = 1e-06
rotary_base = 10000.0
MESH = pl.DeviceIdType.MESH
F32 = jnp.float32
BF16 = jnp.bfloat16


def silu(v):
    return v / (1.0 + jnp.exp(-v))


def rotary_tables(grid_rows):
    pairs = DK // 4
    inverse = (rotary_base ** (-np.arange(pairs, dtype=np.float64) / pairs)).astype(np.float32)

    def tables(count):
        angles = (np.arange(count, dtype=np.float32)[:, None] * inverse[None, :]).astype(np.float32)
        cosine = np.repeat(np.cos(angles.astype(np.float64)), 2, axis=1)
        sine = np.repeat(np.sin(angles.astype(np.float64)), 2, axis=1)
        sine[:, 0::2] *= -1.0
        return cosine.astype(np.float32), sine.astype(np.float32)

    return tables(grid_rows) + tables(GRID_W)


def kernel(
    n_sp, n_tp, group, rows, head_count,
    lat_ref, dec_ref, ctx_ref, cond_ref, ngain_ref, ggain_ref,
    rowc_ref, rows_ref, colc_ref, cols_ref,
    wmod_hbm, wq_hbm, wk_hbm, wv_hbm, wg_hbm, wo_hbm,
    out_ref,
    wmod, wk, wv, wq, wg, wo,
    lat_all, normed, ctx_all, dec_all, mslots, modfull,
    wdec, vecs, etot,
    kbuf, qbuf, vbuf, gbuf, ybuf, fstate, bstate,
    recv_f, recv_b, send_f, send_b,
    pout, pin, psend, pfin,
    w_sem, dec_s, dec_r, m1_s, m1_r, m2_s, m2_r, lat_s, lat_r, rel_s, rel_r,
    ctx_s, ctx_r, ctx_x, f_s, f_r, b_s, b_r, d2d_s, d2d_r, ici_s, ici_r,
):
    sp = lax.axis_index("sp")
    tp = lax.axis_index("tp")
    zz = sp // group
    sub = sp % group
    nz = n_sp // group
    members = group * n_tp
    chips = members // CORES
    me = sub * n_tp + tp
    chip = me // CORES
    core = me % CORES
    tokens = members * rows
    model = lat_ref.shape[1]
    line = chips // group
    at_line = chip % line

    def peer(k, sign=1):
        ds, dx = k // line, k % line
        to_sub = (sub + group + sign * ds) % group
        return to_sub * line + (at_line + line + sign * dx) % line

    straight = [k for k in range(1, chips) if k % line == 0]
    across = [k for k in range(1, chips) if k < line]
    diagonal = [k for k in range(1, chips) if k % line and k >= line]

    def member_device(m):
        return (zz * group + m // n_tp, m % n_tp)

    partner = member_device(chip * CORES + (1 - core))

    def remote(src, dst, ssem, rsem, device):
        return pltpu.make_async_remote_copy(
            src_ref=src, dst_ref=dst, send_sem=ssem, recv_sem=rsem,
            device_id=device, device_id_type=MESH,
        )

    key_cols = pl.ds(pl.multiple_of(sub * DK, DK), DK)
    val_cols = pl.ds(pl.multiple_of(sub * DV, DV), DV)
    loads = [
        pltpu.make_async_copy(wmod_hbm, wmod, w_sem.at[0]),
        pltpu.make_async_copy(wk_hbm.at[:, key_cols], wk, w_sem.at[1]),
        pltpu.make_async_copy(wv_hbm.at[:, val_cols], wv, w_sem.at[2]),
        pltpu.make_async_copy(wq_hbm.at[:, key_cols], wq, w_sem.at[3]),
        pltpu.make_async_copy(wg_hbm.at[:, val_cols], wg, w_sem.at[4]),
        pltpu.make_async_copy(wo_hbm.at[val_cols, :], wo, w_sem.at[5]),
    ]
    for load in loads:
        load.start()

    barrier = pltpu.get_barrier_semaphore()
    greeted = 0
    for d in range(1, n_sp):
        pl.semaphore_signal(
            barrier, inc=1, device_id=((sp + d) % n_sp, tp), device_id_type=MESH
        )
        greeted += 1
    for s in range(group):
        for d in range(1, n_tp):
            pl.semaphore_signal(
                barrier, inc=1, device_id=(zz * group + s, (tp + d) % n_tp), device_id_type=MESH
            )
            greeted += 1
    pl.semaphore_wait(barrier, greeted)

    sends = []

    depth, width = wmod.shape
    if cond_ref.shape[1] == depth:
        own = cond_ref[...]
    else:
        own = cond_ref[:, pl.ds(pl.multiple_of(sp * depth, depth), depth)]
    activated = silu(own.astype(F32)).astype(BF16)
    loads[0].wait()
    mslots[sp] = jnp.dot(activated, wmod[...], preferred_element_type=F32)
    first = []
    for d in range(1, n_sp):
        copy = remote(
            mslots.at[sp], mslots.at[sp], m1_s.at[d], m1_r.at[d], ((sp + d) % n_sp, tp)
        )
        copy.start()
        first.append(copy)
    sends += first

    decay_copies = []
    for d in range(1, group):
        copy = remote(
            dec_ref, dec_all.at[sub], dec_s.at[d], dec_r.at[d],
            (zz * group + (sub + d) % group, tp),
        )
        copy.start()
        decay_copies.append(copy)
    sends += decay_copies
    dec_all[sub] = dec_ref[...]

    lat_copies = {}

    def send_rows(k):
        copy = remote(
            lat_ref, lat_all.at[me], lat_s.at[k], lat_r.at[k],
            member_device(peer(k) * CORES + core),
        )
        copy.start()
        lat_copies[k] = copy
        sends.append(copy)

    for k in straight:
        send_rows(k)
    own_relay = remote(lat_ref, lat_all.at[me], rel_s.at[0], rel_r.at[0], partner)
    own_relay.start()
    sends.append(own_relay)
    lat_all[me] = lat_ref[...]

    ends = sorted({0, nz - 1})
    half = model // CORES
    half_cols = pl.ds(pl.multiple_of(core * half, half), half)
    ctx_sends = []
    for e in ends:
        for s in range(group):
            dest = e * group + s
            slot = len(ctx_sends)

            def ctx_copy(dest=dest, slot=slot):
                return remote(
                    ctx_ref.at[:, half_cols], ctx_all.at[sp, :, half_cols],
                    ctx_s.at[slot], ctx_r.at[sp], (dest, tp),
                )

            @pl.when(sp != dest)
            def _(ctx_copy=ctx_copy):
                ctx_copy().start()

            ctx_sends.append((dest, ctx_copy))
    ctx_all[sp, :, half_cols] = ctx_ref[:, half_cols]

    for copy in first:
        copy.wait_recv()
    total = mslots[0]
    for s in range(1, n_sp):
        total = total + mslots[s]
    mod_cols = pl.ds(pl.multiple_of(tp * width, width), width)
    modfull[:, mod_cols] = total
    second = []
    for d in range(1, n_tp):
        copy = remote(
            modfull.at[:, mod_cols], modfull.at[:, mod_cols], m2_s.at[d], m2_r.at[d],
            (sp, (tp + d) % n_tp),
        )
        copy.start()
        second.append(copy)
    sends += second
    for k in across + diagonal:
        send_rows(k)

    for copy in decay_copies:
        copy.wait_recv()
    head = sub if head_count > 1 else 0
    parts = [dec_all[s, pl.ds(head, 1), :] for s in range(group)]
    a_row = parts[0] if group == 1 else jnp.concatenate(parts, axis=1)
    ii = lax.broadcasted_iota(jnp.int32, (tokens, tokens), 0)
    jj = lax.broadcasted_iota(jnp.int32, (tokens, tokens), 1)
    a_full = jnp.broadcast_to(a_row, (tokens, tokens))
    b_col = jnp.sum(jnp.where(jj <= ii, a_full, 0.0), axis=1, keepdims=True)
    a_col = jnp.sum(jnp.where(jj == ii, a_full, 0.0), axis=1, keepdims=True)
    c_col = b_col - a_col
    b_row = jnp.sum(jnp.where(jj == ii, b_col, 0.0), axis=0, keepdims=True)
    c_row = jnp.sum(jnp.where(jj == ii, c_col, 0.0), axis=0, keepdims=True)
    gap = jnp.where(jj <= ii, b_col - b_row, c_row - c_col)
    wdec[...] = jnp.where(jj == ii, 2.0, jnp.exp(jnp.minimum(gap, 0.0)))
    t_all = b_col[tokens - 1 : tokens, :]
    vecs[0] = jnp.exp(b_col)
    vecs[1] = jnp.exp(t_all - c_col)
    vecs[2] = jnp.exp(t_all - b_col)
    vecs[3] = jnp.exp(c_col)
    etot[...] = jnp.broadcast_to(jnp.exp(t_all), etot.shape)

    for copy in second:
        copy.wait_recv()
    gain = ngain_ref[...].astype(F32).reshape(1, -1)

    def modulate(x, row):
        wide = x.astype(F32)
        normal = wide * lax.rsqrt(jnp.mean(wide * wide, axis=-1, keepdims=True) + epsilon)
        shift = modfull[row : row + 1, 0:model]
        scale = modfull[row : row + 1, model : 2 * model]
        return (normal * gain * (1.0 + scale) + shift).astype(BF16)

    def normalise(m):
        normed[m] = modulate(lat_all[m], 0)

    def arrive(k):
        mine = peer(k, -1) * CORES + core
        other = peer(k, -1) * CORES + (1 - core)
        relay = own_relay
        if k:
            lat_copies[k].wait_recv()
            relay = remote(lat_all.at[mine], lat_all.at[mine], rel_s.at[k], rel_r.at[k], partner)
            relay.start()
            sends.append(relay)
        normalise(mine)
        relay.wait_recv()
        normalise(other)

    for k in [0] + straight + across:
        arrive(k)

    loads[1].wait()
    loads[2].wait()
    over_tokens = (((0,), (0,)), ((), ()))
    end = (zz == 0) | (zz == nz - 1)
    lower = 2 * zz < nz

    @pl.when(end)
    def _():
        for s in range(n_sp):
            @pl.when(sp != s)
            def _(s=s):
                remote(
                    ctx_ref.at[:, half_cols], ctx_all.at[s, :, half_cols],
                    ctx_s.at[0], ctx_r.at[s], partner,
                ).wait_recv()
        swap = remote(
            ctx_all.at[:, :, half_cols], ctx_all.at[:, :, half_cols],
            ctx_x.at[0], ctx_x.at[1], partner,
        )
        swap.start()
        swap.wait()
        cn = modulate(ctx_all[...].reshape(-1, model), 1)
        ck = (jnp.dot(cn, wk[...], preferred_element_type=F32) * DK ** (-0.5)).astype(BF16)
        cv = jnp.dot(cn, wv[...], preferred_element_type=F32).astype(BF16)
        state = lax.dot_general(ck, cv, over_tokens, preferred_element_type=F32) * float(CTX_LIFT)
        state = state.astype(BF16).reshape(recv_f.shape)

        @pl.when(zz == 0)
        def _():
            recv_f[...] = state

        @pl.when(zz == nz - 1)
        def _():
            recv_b[...] = state

    for k in diagonal:
        arrive(k)

    x = normed[...].reshape(tokens, model)
    lanes = lax.broadcasted_iota(jnp.int32, (GRID_W, DK // 2), 1)
    even = lanes % 2 == 0
    row_base = zz * (tokens // GRID_W)

    def rotate_into(dst, scale):
        for r in range(tokens // GRID_W):
            at = slice(r * GRID_W, (r + 1) * GRID_W)
            row_c = rowc_ref[pl.ds(row_base + r, 1), :]
            row_s = rows_ref[pl.ds(row_base + r, 1), :]
            for part in range(2):
                cut = slice(part * (DK // 2), (part + 1) * (DK // 2))
                u = ybuf[at, cut]
                swapped = jnp.where(
                    even, pltpu.roll(u, DK // 2 - 1, 1), pltpu.roll(u, 1, 1)
                )
                if part == 0:
                    turned = u * row_c + swapped * row_s
                else:
                    turned = u * colc_ref[...] + swapped * cols_ref[...]
                dst[at, cut] = (turned * scale).astype(BF16)

    ybuf[:, 0:DK] = jnp.dot(x, wk[...], preferred_element_type=F32)
    rotate_into(kbuf, DK ** (-0.5))
    for n in range(DV // 256):
        cut = slice(n * 256, (n + 1) * 256)
        vbuf[:, cut] = jnp.dot(x, wv[:, cut], preferred_element_type=F32).astype(BF16)

    v = vbuf[...]
    kw = kbuf[...].astype(F32)
    fstate[...] = lax.dot_general(
        (kw * vecs[2]).astype(BF16), v, over_tokens, preferred_element_type=F32
    )
    bstate[...] = lax.dot_general(
        (kw * vecs[3]).astype(BF16), v, over_tokens, preferred_element_type=F32
    )

    piece = DK // CHUNKS

    def f_copy(c):
        return remote(
            send_f.at[c], recv_f.at[c], f_s.at[c], f_r.at[c], ((sp + group) % n_sp, tp)
        )

    def b_copy(c):
        return remote(
            send_b.at[c], recv_b.at[c], b_s.at[c], b_r.at[c], ((sp + n_sp - group) % n_sp, tp)
        )

    def chain_f():
        for c in range(CHUNKS):
            @pl.when(zz > 0)
            def _(c=c):
                f_copy(c).wait_recv()

            @pl.when(zz < nz - 1)
            def _(c=c):
                cut = slice(c * piece, (c + 1) * piece)
                send_f[c] = (etot[...] * recv_f[c].astype(F32) + fstate[cut, :]).astype(BF16)
                f_copy(c).start()

    def chain_b():
        for c in range(CHUNKS):
            @pl.when(zz < nz - 1)
            def _(c=c):
                b_copy(c).wait_recv()

            @pl.when(zz > 0)
            def _(c=c):
                cut = slice(c * piece, (c + 1) * piece)
                send_b[c] = (etot[...] * recv_b[c].astype(F32) + bstate[cut, :]).astype(BF16)
                b_copy(c).start()

    def chain(where, forward_if):
        @pl.when(where & forward_if)
        def _():
            chain_f()

        @pl.when(where & jnp.logical_not(forward_if))
        def _():
            chain_b()

    middle = jnp.logical_not(end)
    upper = jnp.logical_not(lower)
    chain(end, lower)
    loads[3].wait()
    ybuf[:, 0:DK] = jnp.dot(x, wq[...], preferred_element_type=F32)
    rotate_into(qbuf, 1.0)
    chain(middle, lower)
    scores = lax.dot_general(
        qbuf[...], kbuf[...], (((1,), (1,)), ((), ())), preferred_element_type=F32
    )
    ybuf[...] = jnp.dot((scores * wdec[...]).astype(BF16), v, preferred_element_type=F32)
    chain(middle, upper)
    loads[4].wait()
    gains = ggain_ref[...].astype(F32).reshape(head_count, DV)
    group_row = gains[0:1]
    for h in range(1, head_count):
        group_row = jnp.where(sub == h, gains[h : h + 1], group_row)
    for n in range(DV // 256):
        cut = slice(n * 256, (n + 1) * 256)
        g = jnp.dot(x, wg[:, cut], preferred_element_type=F32).astype(BF16)
        gbuf[:, cut] = silu(g.astype(F32)) * group_row[:, cut]
    chain(end, upper)

    loads[5].wait()
    order = diagonal + across + straight + [0]
    pair_copies = {}
    final = {}

    def finish(d):
        pair_copies[d].wait_recv()
        both = pout[d, core].astype(F32) + pin[d].astype(F32)
        if d == 0:
            final["own"] = both
            return
        psend[d] = both.astype(BF16)
        copy = remote(
            psend.at[d], pfin.at[d], ici_s.at[d], ici_r.at[d],
            member_device(peer(d) * CORES + core),
        )
        copy.start()
        final[d] = copy
        sends.append(copy)

    span = CORES * rows

    def attend(c):
        at = pl.ds(pl.multiple_of(c * span, span), span)
        q = qbuf[at, :]
        y = ybuf[at, :]
        y = y + vecs[0, at, :] * jnp.dot(
            q, recv_f[...].reshape(DK, DV), preferred_element_type=F32
        )
        y = y + vecs[1, at, :] * jnp.dot(
            q, recv_b[...].reshape(DK, DV), preferred_element_type=F32
        )
        centred = y - jnp.mean(y, axis=-1, keepdims=True)
        variance = jnp.mean(centred * centred, axis=-1, keepdims=True)
        return (gbuf[at, :] * (centred * lax.rsqrt(variance + epsilon))).astype(BF16)

    for place, d in enumerate(order):
        rows_of = attend(peer(d))
        pout[d] = (
            jnp.dot(rows_of, wo[...], preferred_element_type=F32)
            .astype(BF16)
            .reshape(CORES, rows, model)
        )
        copy = remote(pout.at[d, 1 - core], pin.at[d], d2d_s.at[d], d2d_r.at[d], partner)
        copy.start()
        pair_copies[d] = copy
        sends.append(copy)
        if place:
            finish(order[place - 1])
    finish(order[-1])
    acc = final["own"]
    for d in range(1, chips):
        final[d].wait_recv()
        acc = acc + pfin[d].astype(F32)
    gate = modfull[0:1, 2 * model : 3 * model]
    out_ref[...] = (lat_ref[...].astype(F32) + gate * acc).astype(BF16)

    for copy in sends:
        copy.wait_send()
    for dest, ctx_copy in ctx_sends:
        @pl.when(sp != dest)
        def _(ctx_copy=ctx_copy):
            ctx_copy().wait_send()

    @pl.when(zz < nz - 1)
    def _():
        for c in range(CHUNKS):
            f_copy(c).wait_send()

    @pl.when(zz > 0)
    def _():
        for c in range(CHUNKS):
            b_copy(c).wait_send()


def per_device(
    n_sp, n_tp,
    latent, log_decay, context, condition, w_modulate, norm_gain,
    w_query, w_key, w_value, w_gate, group_gain, w_output,
):
    rows, model = latent.shape
    head_count = w_query.shape[1] // DK
    group = head_count
    members = group * n_tp
    chips = members // CORES
    tokens = members * rows
    depth, width = w_modulate.shape
    ctx_rows = context.shape[0]
    if depth % 128:
        condition = lax.dynamic_slice_in_dim(condition, lax.axis_index("sp") * depth, depth, 1)
    total_rows = rows * n_sp * n_tp
    tables = [jnp.asarray(t) for t in rotary_tables(total_rows // GRID_W)]
    vmem = pl.BlockSpec(memory_space=pltpu.VMEM)
    hbm = pl.BlockSpec(memory_space=pl.ANY)
    sem = pltpu.SemaphoreType.DMA
    ends = 2 * group
    scratch = [
        pltpu.VMEM((depth, width), BF16),
        pltpu.VMEM((model, DK), BF16),
        pltpu.VMEM((model, DV), BF16),
        pltpu.VMEM((model, DK), BF16),
        pltpu.VMEM((model, DV), BF16),
        pltpu.VMEM((DV, model), BF16),
        pltpu.VMEM((members, rows, model), BF16),
        pltpu.VMEM((members, rows, model), BF16),
        pltpu.VMEM((n_sp, ctx_rows, model), BF16),
        pltpu.VMEM((group, head_count, log_decay.shape[0]), F32),
        pltpu.VMEM((n_sp, condition.shape[0], width), F32),
        pltpu.VMEM((condition.shape[0], width * n_tp), F32),
        pltpu.VMEM((tokens, tokens), F32),
        pltpu.VMEM((4, tokens, 1), F32),
        pltpu.VMEM((1, DV), F32),
        pltpu.VMEM((tokens, DK), BF16),
        pltpu.VMEM((tokens, DK), BF16),
        pltpu.VMEM((tokens, DV), BF16),
        pltpu.VMEM((tokens, DV), F32),
        pltpu.VMEM((tokens, DV), F32),
        pltpu.VMEM((DK, DV), F32),
        pltpu.VMEM((DK, DV), F32),
        pltpu.VMEM((CHUNKS, DK // CHUNKS, DV), BF16),
        pltpu.VMEM((CHUNKS, DK // CHUNKS, DV), BF16),
        pltpu.VMEM((CHUNKS, DK // CHUNKS, DV), BF16),
        pltpu.VMEM((CHUNKS, DK // CHUNKS, DV), BF16),
        pltpu.VMEM((chips, CORES, rows, model), BF16),
        pltpu.VMEM((chips, rows, model), BF16),
        pltpu.VMEM((chips, rows, model), BF16),
        pltpu.VMEM((chips, rows, model), BF16),
        sem((6,)),
        sem((group,)), sem((group,)),
        sem((n_sp,)), sem((n_sp,)),
        sem((n_tp,)), sem((n_tp,)),
        sem((chips,)), sem((chips,)),
        sem((chips,)), sem((chips,)),
        sem((ends,)), sem((n_sp,)), sem((2,)),
        sem((CHUNKS,)), sem((CHUNKS,)),
        sem((CHUNKS,)), sem((CHUNKS,)),
        sem((chips,)), sem((chips,)),
        sem((chips,)), sem((chips,)),
    ]
    return pl.pallas_call(
        functools.partial(kernel, n_sp, n_tp, group, rows, head_count),
        out_shape=jax.ShapeDtypeStruct((rows, model), BF16),
        in_specs=[vmem] * 10 + [hbm] * 6,
        out_specs=vmem,
        scratch_shapes=scratch,
        compiler_params=pltpu.CompilerParams(
            collective_id=0, has_side_effects=True, vmem_limit_bytes=58 * 1024 * 1024
        ),
    )(
        latent, log_decay.T, context, condition,
        norm_gain, group_gain,
        *tables,
        w_modulate, w_query, w_key, w_value, w_gate, w_output,
    )


def solution(mesh):
    placed = (
        P(("sp", "tp"), None),
        P("sp", "tp"),
        P("sp", None),
        P(),
        P("sp", "tp"),
        P(),
        P(None, "tp"),
        P(None, "tp"),
        P(None, "tp"),
        P(None, "tp"),
        P("tp"),
        P("tp", None),
    )
    body = functools.partial(per_device, mesh.shape["sp"], mesh.shape["tp"])
    return jax.shard_map(
        body, mesh=mesh, in_specs=placed, out_specs=P(("sp", "tp"), None), check_vma=False
    )
```

```python
import functools

import jax
import jax.numpy as jnp
import numpy as np
from jax import lax
from jax.experimental import pallas as pl
from jax.experimental.pallas import tpu as pltpu
from jax.sharding import PartitionSpec as P

DK = 256
DV = 512
GRID_W = 64
CTX_LIFT = 4
CORES = 2
CHUNKS = 8

epsilon = 1e-06
rotary_base = 10000.0
MESH = pl.DeviceIdType.MESH
F32 = jnp.float32
BF16 = jnp.bfloat16


def silu(v):
    return v / (1.0 + jnp.exp(-v))


def rotary_tables(grid_rows):
    pairs = DK // 4
    inverse = (rotary_base ** (-np.arange(pairs, dtype=np.float64) / pairs)).astype(np.float32)

    def tables(count):
        angles = (np.arange(count, dtype=np.float32)[:, None] * inverse[None, :]).astype(np.float32)
        cosine = np.repeat(np.cos(angles.astype(np.float64)), 2, axis=1)
        sine = np.repeat(np.sin(angles.astype(np.float64)), 2, axis=1)
        sine[:, 0::2] *= -1.0
        return cosine.astype(np.float32), sine.astype(np.float32)

    return tables(grid_rows) + tables(GRID_W)


def kernel(
    n_sp, n_tp, group, rows, head_count,
    lat_ref, dec_ref, ctx_ref, cond_ref, ngain_ref, ggain_ref,
    rowc_ref, rows_ref, colc_ref, cols_ref,
    wmod_hbm, wq_hbm, wk_hbm, wv_hbm, wg_hbm, wo_hbm,
    out_ref,
    wmod, wk, wv, wq, wg, wo,
    lat_all, normed, ctx_all, dec_all, mslots, modfull,
    wdec, vecs, etot,
    kbuf, qbuf, vbuf, gbuf, ybuf, fstate, bstate,
    recv_f, recv_b, send_f, send_b,
    pout, pin, psend, pfin,
    w_sem, dec_s, dec_r, m1_s, m1_r, m2_s, m2_r, lat_s, lat_r, rel_s, rel_r,
    ctx_s, ctx_r, ctx_x, f_s, f_r, b_s, b_r, d2d_s, d2d_r, ici_s, ici_r,
):
    sp = lax.axis_index("sp")
    tp = lax.axis_index("tp")
    zz = sp // group
    sub = sp % group
    nz = n_sp // group
    members = group * n_tp
    chips = members // CORES
    me = sub * n_tp + tp
    chip = me // CORES
    core = me % CORES
    tokens = members * rows
    model = lat_ref.shape[1]
    line = chips // group
    at_line = chip % line

    def peer(k, sign=1):
        ds, dx = k // line, k % line
        to_sub = (sub + group + sign * ds) % group
        return to_sub * line + (at_line + line + sign * dx) % line

    straight = [k for k in range(1, chips) if k % line == 0]
    across = [k for k in range(1, chips) if k < line]
    diagonal = [k for k in range(1, chips) if k % line and k >= line]

    def member_device(m):
        return (zz * group + m // n_tp, m % n_tp)

    partner = member_device(chip * CORES + (1 - core))

    def remote(src, dst, ssem, rsem, device):
        return pltpu.make_async_remote_copy(
            src_ref=src, dst_ref=dst, send_sem=ssem, recv_sem=rsem,
            device_id=device, device_id_type=MESH,
        )

    key_cols = pl.ds(pl.multiple_of(sub * DK, DK), DK)
    val_cols = pl.ds(pl.multiple_of(sub * DV, DV), DV)
    loads = [
        pltpu.make_async_copy(wmod_hbm, wmod, w_sem.at[0]),
        pltpu.make_async_copy(wk_hbm.at[:, key_cols], wk, w_sem.at[1]),
        pltpu.make_async_copy(wv_hbm.at[:, val_cols], wv, w_sem.at[2]),
        pltpu.make_async_copy(wq_hbm.at[:, key_cols], wq, w_sem.at[3]),
        pltpu.make_async_copy(wg_hbm.at[:, val_cols], wg, w_sem.at[4]),
        pltpu.make_async_copy(wo_hbm.at[val_cols, :], wo, w_sem.at[5]),
    ]
    for load in loads:
        load.start()

    barrier = pltpu.get_barrier_semaphore()
    greeted = 0
    for d in range(1, n_sp):
        pl.semaphore_signal(
            barrier, inc=1, device_id=((sp + d) % n_sp, tp), device_id_type=MESH
        )
        greeted += 1
    for s in range(group):
        for d in range(1, n_tp):
            pl.semaphore_signal(
                barrier, inc=1, device_id=(zz * group + s, (tp + d) % n_tp), device_id_type=MESH
            )
            greeted += 1
    pl.semaphore_wait(barrier, greeted)

    sends = []

    depth, width = wmod.shape
    if cond_ref.shape[1] == depth:
        own = cond_ref[...]
    else:
        own = cond_ref[:, pl.ds(pl.multiple_of(sp * depth, depth), depth)]
    activated = silu(own.astype(F32)).astype(BF16)
    loads[0].wait()
    mslots[sp] = jnp.dot(activated, wmod[...], preferred_element_type=F32)
    first = []
    for d in range(1, n_sp):
        copy = remote(
            mslots.at[sp], mslots.at[sp], m1_s.at[d], m1_r.at[d], ((sp + d) % n_sp, tp)
        )
        copy.start()
        first.append(copy)
    sends += first

    decay_copies = []
    for d in range(1, group):
        copy = remote(
            dec_ref, dec_all.at[sub], dec_s.at[d], dec_r.at[d],
            (zz * group + (sub + d) % group, tp),
        )
        copy.start()
        decay_copies.append(copy)
    sends += decay_copies
    dec_all[sub] = dec_ref[...]

    lat_copies = {}

    def send_rows(k):
        copy = remote(
            lat_ref, lat_all.at[me], lat_s.at[k], lat_r.at[k],
            member_device(peer(k) * CORES + core),
        )
        copy.start()
        lat_copies[k] = copy
        sends.append(copy)

    for k in straight:
        send_rows(k)
    own_relay = remote(lat_ref, lat_all.at[me], rel_s.at[0], rel_r.at[0], partner)
    own_relay.start()
    sends.append(own_relay)
    lat_all[me] = lat_ref[...]

    ends = sorted({0, nz - 1})
    half = model // CORES
    half_cols = pl.ds(pl.multiple_of(core * half, half), half)
    ctx_sends = []
    for e in ends:
        for s in range(group):
            dest = e * group + s
            slot = len(ctx_sends)

            def ctx_copy(dest=dest, slot=slot):
                return remote(
                    ctx_ref.at[:, half_cols], ctx_all.at[sp, :, half_cols],
                    ctx_s.at[slot], ctx_r.at[sp], (dest, tp),
                )

            @pl.when(sp != dest)
            def _(ctx_copy=ctx_copy):
                ctx_copy().start()

            ctx_sends.append((dest, ctx_copy))
    ctx_all[sp, :, half_cols] = ctx_ref[:, half_cols]

    for copy in first:
        copy.wait_recv()
    total = mslots[0]
    for s in range(1, n_sp):
        total = total + mslots[s]
    mod_cols = pl.ds(pl.multiple_of(tp * width, width), width)
    modfull[:, mod_cols] = total
    second = []
    for d in range(1, n_tp):
        copy = remote(
            modfull.at[:, mod_cols], modfull.at[:, mod_cols], m2_s.at[d], m2_r.at[d],
            (sp, (tp + d) % n_tp),
        )
        copy.start()
        second.append(copy)
    sends += second
    for k in across + diagonal:
        send_rows(k)

    for copy in decay_copies:
        copy.wait_recv()
    head = sub if head_count > 1 else 0
    parts = [dec_all[s, pl.ds(head, 1), :] for s in range(group)]
    a_row = parts[0] if group == 1 else jnp.concatenate(parts, axis=1)
    ii = lax.broadcasted_iota(jnp.int32, (tokens, tokens), 0)
    jj = lax.broadcasted_iota(jnp.int32, (tokens, tokens), 1)
    a_full = jnp.broadcast_to(a_row, (tokens, tokens))
    b_col = jnp.sum(jnp.where(jj <= ii, a_full, 0.0), axis=1, keepdims=True)
    a_col = jnp.sum(jnp.where(jj == ii, a_full, 0.0), axis=1, keepdims=True)
    c_col = b_col - a_col
    b_row = jnp.sum(jnp.where(jj == ii, b_col, 0.0), axis=0, keepdims=True)
    c_row = jnp.sum(jnp.where(jj == ii, c_col, 0.0), axis=0, keepdims=True)
    gap = jnp.where(jj <= ii, b_col - b_row, c_row - c_col)
    wdec[...] = jnp.where(jj == ii, 2.0, jnp.exp(jnp.minimum(gap, 0.0)))
    t_all = b_col[tokens - 1 : tokens, :]
    vecs[0] = jnp.exp(b_col)
    vecs[1] = jnp.exp(t_all - c_col)
    vecs[2] = jnp.exp(t_all - b_col)
    vecs[3] = jnp.exp(c_col)
    etot[...] = jnp.broadcast_to(jnp.exp(t_all), etot.shape)

    for copy in second:
        copy.wait_recv()
    gain = ngain_ref[...].astype(F32).reshape(1, -1)

    def modulate(x, row):
        wide = x.astype(F32)
        normal = wide * lax.rsqrt(jnp.mean(wide * wide, axis=-1, keepdims=True) + epsilon)
        shift = modfull[row : row + 1, 0:model]
        scale = modfull[row : row + 1, model : 2 * model]
        return (normal * gain * (1.0 + scale) + shift).astype(BF16)

    def normalise(m):
        normed[m] = modulate(lat_all[m], 0)

    def arrive(k):
        mine = peer(k, -1) * CORES + core
        other = peer(k, -1) * CORES + (1 - core)
        relay = own_relay
        if k:
            lat_copies[k].wait_recv()
            relay = remote(lat_all.at[mine], lat_all.at[mine], rel_s.at[k], rel_r.at[k], partner)
            relay.start()
            sends.append(relay)
        normalise(mine)
        relay.wait_recv()
        normalise(other)

    for k in [0] + straight + across:
        arrive(k)

    loads[1].wait()
    loads[2].wait()
    over_tokens = (((0,), (0,)), ((), ()))
    end = (zz == 0) | (zz == nz - 1)
    lower = 2 * zz < nz

    @pl.when(end)
    def _():
        for s in range(n_sp):
            @pl.when(sp != s)
            def _(s=s):
                remote(
                    ctx_ref.at[:, half_cols], ctx_all.at[s, :, half_cols],
                    ctx_s.at[0], ctx_r.at[s], partner,
                ).wait_recv()
        swap = remote(
            ctx_all.at[:, :, half_cols], ctx_all.at[:, :, half_cols],
            ctx_x.at[0], ctx_x.at[1], partner,
        )
        swap.start()
        swap.wait()
        cn = modulate(ctx_all[...].reshape(-1, model), 1)
        ck = (jnp.dot(cn, wk[...], preferred_element_type=F32) * DK ** (-0.5)).astype(BF16)
        cv = jnp.dot(cn, wv[...], preferred_element_type=F32).astype(BF16)
        state = lax.dot_general(ck, cv, over_tokens, preferred_element_type=F32) * float(CTX_LIFT)
        state = state.astype(BF16).reshape(recv_f.shape)

        @pl.when(zz == 0)
        def _():
            recv_f[...] = state

        @pl.when(zz == nz - 1)
        def _():
            recv_b[...] = state

    for k in diagonal:
        arrive(k)

    x = normed[...].reshape(tokens, model)
    lanes = lax.broadcasted_iota(jnp.int32, (GRID_W, DK // 2), 1)
    even = lanes % 2 == 0
    row_base = zz * (tokens // GRID_W)

    def rotate_into(dst, scale):
        for r in range(tokens // GRID_W):
            at = slice(r * GRID_W, (r + 1) * GRID_W)
            row_c = rowc_ref[pl.ds(row_base + r, 1), :]
            row_s = rows_ref[pl.ds(row_base + r, 1), :]
            for part in range(2):
                cut = slice(part * (DK // 2), (part + 1) * (DK // 2))
                u = ybuf[at, cut]
                swapped = jnp.where(
                    even, pltpu.roll(u, DK // 2 - 1, 1), pltpu.roll(u, 1, 1)
                )
                if part == 0:
                    turned = u * row_c + swapped * row_s
                else:
                    turned = u * colc_ref[...] + swapped * cols_ref[...]
                dst[at, cut] = (turned * scale).astype(BF16)

    ybuf[:, 0:DK] = jnp.dot(x, wk[...], preferred_element_type=F32)
    rotate_into(kbuf, DK ** (-0.5))
    for n in range(DV // 256):
        cut = slice(n * 256, (n + 1) * 256)
        vbuf[:, cut] = jnp.dot(x, wv[:, cut], preferred_element_type=F32).astype(BF16)

    v = vbuf[...]
    kw = kbuf[...].astype(F32)
    fstate[...] = lax.dot_general(
        (kw * vecs[2]).astype(BF16), v, over_tokens, preferred_element_type=F32
    )
    bstate[...] = lax.dot_general(
        (kw * vecs[3]).astype(BF16), v, over_tokens, preferred_element_type=F32
    )

    piece = DK // CHUNKS

    def f_copy(c):
        return remote(
            send_f.at[c], recv_f.at[c], f_s.at[c], f_r.at[c], ((sp + group) % n_sp, tp)
        )

    def b_copy(c):
        return remote(
            send_b.at[c], recv_b.at[c], b_s.at[c], b_r.at[c], ((sp + n_sp - group) % n_sp, tp)
        )

    def chain_f():
        for c in range(CHUNKS):
            @pl.when(zz > 0)
            def _(c=c):
                f_copy(c).wait_recv()

            @pl.when(zz < nz - 1)
            def _(c=c):
                cut = slice(c * piece, (c + 1) * piece)
                send_f[c] = (etot[...] * recv_f[c].astype(F32) + fstate[cut, :]).astype(BF16)
                f_copy(c).start()

    def chain_b():
        for c in range(CHUNKS):
            @pl.when(zz < nz - 1)
            def _(c=c):
                b_copy(c).wait_recv()

            @pl.when(zz > 0)
            def _(c=c):
                cut = slice(c * piece, (c + 1) * piece)
                send_b[c] = (etot[...] * recv_b[c].astype(F32) + bstate[cut, :]).astype(BF16)
                b_copy(c).start()

    def chain(where, forward_if):
        @pl.when(where & forward_if)
        def _():
            chain_f()

        @pl.when(where & jnp.logical_not(forward_if))
        def _():
            chain_b()

    middle = jnp.logical_not(end)
    upper = jnp.logical_not(lower)
    chain(end, lower)
    loads[3].wait()
    ybuf[:, 0:DK] = jnp.dot(x, wq[...], preferred_element_type=F32)
    rotate_into(qbuf, 1.0)
    chain(middle, lower)
    scores = lax.dot_general(
        qbuf[...], kbuf[...], (((1,), (1,)), ((), ())), preferred_element_type=F32
    )
    ybuf[...] = jnp.dot((scores * wdec[...]).astype(BF16), v, preferred_element_type=F32)
    chain(middle, upper)
    loads[4].wait()
    gains = ggain_ref[...].astype(F32).reshape(head_count, DV)
    group_row = gains[0:1]
    for h in range(1, head_count):
        group_row = jnp.where(sub == h, gains[h : h + 1], group_row)
    for n in range(DV // 256):
        cut = slice(n * 256, (n + 1) * 256)
        g = jnp.dot(x, wg[:, cut], preferred_element_type=F32).astype(BF16)
        gbuf[:, cut] = silu(g.astype(F32)) * group_row[:, cut]
    chain(end, upper)

    loads[5].wait()
    order = diagonal + across + straight + [0]
    pair_copies = {}
    final = {}

    def finish(d):
        pair_copies[d].wait_recv()
        both = pout[d, core].astype(F32) + pin[d].astype(F32)
        if d == 0:
            final["own"] = both
            return
        psend[d] = both.astype(BF16)
        copy = remote(
            psend.at[d], pfin.at[d], ici_s.at[d], ici_r.at[d],
            member_device(peer(d) * CORES + core),
        )
        copy.start()
        final[d] = copy
        sends.append(copy)

    span = CORES * rows

    def attend(c):
        at = pl.ds(pl.multiple_of(c * span, span), span)
        q = qbuf[at, :]
        y = ybuf[at, :]
        y = y + vecs[0, at, :] * jnp.dot(
            q, recv_f[...].reshape(DK, DV), preferred_element_type=F32
        )
        y = y + vecs[1, at, :] * jnp.dot(
            q, recv_b[...].reshape(DK, DV), preferred_element_type=F32
        )
        centred = y - jnp.mean(y, axis=-1, keepdims=True)
        variance = jnp.mean(centred * centred, axis=-1, keepdims=True)
        return (gbuf[at, :] * (centred * lax.rsqrt(variance + epsilon))).astype(BF16)

    for place, d in enumerate(order):
        rows_of = attend(peer(d))
        pout[d] = (
            jnp.dot(rows_of, wo[...], preferred_element_type=F32)
            .astype(BF16)
            .reshape(CORES, rows, model)
        )
        copy = remote(pout.at[d, 1 - core], pin.at[d], d2d_s.at[d], d2d_r.at[d], partner)
        copy.start()
        pair_copies[d] = copy
        sends.append(copy)
        if place:
            finish(order[place - 1])
    finish(order[-1])
    acc = final["own"]
    for d in range(1, chips):
        final[d].wait_recv()
        acc = acc + pfin[d].astype(F32)
    gate = modfull[0:1, 2 * model : 3 * model]
    out_ref[...] = (lat_ref[...].astype(F32) + gate * acc).astype(BF16)

    for copy in sends:
        copy.wait_send()
    for dest, ctx_copy in ctx_sends:
        @pl.when(sp != dest)
        def _(ctx_copy=ctx_copy):
            ctx_copy().wait_send()

    @pl.when(zz < nz - 1)
    def _():
        for c in range(CHUNKS):
            f_copy(c).wait_send()

    @pl.when(zz > 0)
    def _():
        for c in range(CHUNKS):
            b_copy(c).wait_send()


def per_device(
    n_sp, n_tp,
    latent, log_decay, context, condition, w_modulate, norm_gain,
    w_query, w_key, w_value, w_gate, group_gain, w_output,
):
    rows, model = latent.shape
    head_count = w_query.shape[1] // DK
    group = head_count
    members = group * n_tp
    chips = members // CORES
    tokens = members * rows
    depth, width = w_modulate.shape
    ctx_rows = context.shape[0]
    if depth % 128:
        condition = lax.dynamic_slice_in_dim(condition, lax.axis_index("sp") * depth, depth, 1)
    total_rows = rows * n_sp * n_tp
    tables = [jnp.asarray(t) for t in rotary_tables(total_rows // GRID_W)]
    vmem = pl.BlockSpec(memory_space=pltpu.VMEM)
    hbm = pl.BlockSpec(memory_space=pl.ANY)
    sem = pltpu.SemaphoreType.DMA
    ends = 2 * group
    scratch = [
        pltpu.VMEM((depth, width), BF16),
        pltpu.VMEM((model, DK), BF16),
        pltpu.VMEM((model, DV), BF16),
        pltpu.VMEM((model, DK), BF16),
        pltpu.VMEM((model, DV), BF16),
        pltpu.VMEM((DV, model), BF16),
        pltpu.VMEM((members, rows, model), BF16),
        pltpu.VMEM((members, rows, model), BF16),
        pltpu.VMEM((n_sp, ctx_rows, model), BF16),
        pltpu.VMEM((group, head_count, log_decay.shape[0]), F32),
        pltpu.VMEM((n_sp, condition.shape[0], width), F32),
        pltpu.VMEM((condition.shape[0], width * n_tp), F32),
        pltpu.VMEM((tokens, tokens), F32),
        pltpu.VMEM((4, tokens, 1), F32),
        pltpu.VMEM((1, DV), F32),
        pltpu.VMEM((tokens, DK), BF16),
        pltpu.VMEM((tokens, DK), BF16),
        pltpu.VMEM((tokens, DV), BF16),
        pltpu.VMEM((tokens, DV), F32),
        pltpu.VMEM((tokens, DV), F32),
        pltpu.VMEM((DK, DV), F32),
        pltpu.VMEM((DK, DV), F32),
        pltpu.VMEM((CHUNKS, DK // CHUNKS, DV), BF16),
        pltpu.VMEM((CHUNKS, DK // CHUNKS, DV), BF16),
        pltpu.VMEM((CHUNKS, DK // CHUNKS, DV), BF16),
        pltpu.VMEM((CHUNKS, DK // CHUNKS, DV), BF16),
        pltpu.VMEM((chips, CORES, rows, model), BF16),
        pltpu.VMEM((chips, rows, model), BF16),
        pltpu.VMEM((chips, rows, model), BF16),
        pltpu.VMEM((chips, rows, model), BF16),
        sem((6,)),
        sem((group,)), sem((group,)),
        sem((n_sp,)), sem((n_sp,)),
        sem((n_tp,)), sem((n_tp,)),
        sem((chips,)), sem((chips,)),
        sem((chips,)), sem((chips,)),
        sem((ends,)), sem((n_sp,)), sem((2,)),
        sem((CHUNKS,)), sem((CHUNKS,)),
        sem((CHUNKS,)), sem((CHUNKS,)),
        sem((chips,)), sem((chips,)),
        sem((chips,)), sem((chips,)),
    ]
    return pl.pallas_call(
        functools.partial(kernel, n_sp, n_tp, group, rows, head_count),
        out_shape=jax.ShapeDtypeStruct((rows, model), BF16),
        in_specs=[vmem] * 10 + [hbm] * 6,
        out_specs=vmem,
        scratch_shapes=scratch,
        compiler_params=pltpu.CompilerParams(
            collective_id=0, has_side_effects=True, vmem_limit_bytes=58 * 1024 * 1024
        ),
    )(
        latent, log_decay.T, context, condition,
        norm_gain, group_gain,
        *tables,
        w_modulate, w_query, w_key, w_value, w_gate, w_output,
    )


def solution(mesh):
    placed = (
        P(("sp", "tp"), None),
        P("sp", "tp"),
        P("sp", None),
        P(),
        P("sp", "tp"),
        P(),
        P(None, "tp"),
        P(None, "tp"),
        P(None, "tp"),
        P(None, "tp"),
        P("tp"),
        P("tp", None),
    )
    body = functools.partial(per_device, mesh.shape["sp"], mesh.shape["tp"])
    return jax.shard_map(
        body, mesh=mesh, in_specs=placed, out_specs=P(("sp", "tp"), None), check_vma=False
    )
```
